32 devices in a mesh: sp: 8 (over z, x), tp: 4 (over y, core).
Axes of the slice: x: 2, y: 2, z: 4, core: 2. Of those that a mesh axis runs over, the one named last changes fastest.
Arguments:
- token_grid: bfloat16 [8, 2048, 512], P('sp', 'tp'), may hold values from -6 to 6
- norm_gain: bfloat16 [3, 2048], replicated, may hold values from 0.099609375 to 1.8984375
- w_query: bfloat16 [3, 2048, 2048], P(None, None, 'tp'), may hold values from -0.125 to 0.125
- w_key: bfloat16 [3, 2048, 2048], P(None, None, 'tp'), may hold values from -0.125 to 0.125
- w_value: bfloat16 [3, 2048, 2048], P(None, None, 'tp'), may hold values from -0.125 to 0.125
- w_out: bfloat16 [3, 2048, 2048], P(None, 'tp'), may hold values from -0.5 to 0.5
- rel_bias: float32 [3, 32, 8, 16], P(None, 'tp'), may hold values from -3 to 250
Outputs:
- grid_out: bfloat16 [8, 2048, 512], P('sp', 'tp')
The draws below stay inside these ranges and needn't reach their ends.
All inputs are finite; a program needn't handle non-finite values.
Results may differ from the reference program's by a relative error of at most 0.024.
Values may be sent and summed in bfloat16 or wider, within the bound.
A program may use at most 128 MiB of HBM per device.

```python
import jax
import jax.numpy as jnp
from jax import lax

D = 2048
HEADS = 32
HEAD_DIM = 64
WIN_R = 8
WIN_C = 16
LAYERS = 3
COLS = 512
ROWS = 8
N_TP = 4


def draw_rel_bias(key, part):
    dims_all = (LAYERS, HEADS, WIN_R, WIN_C)
    baseline = jnp.clip(jax.random.normal(jax.random.fold_in(key, 11), dims_all, jnp.float32), -3.0, 3.0)
    return baseline


def block_scale(own_key, shape, shards, low, high):
    def one(axis_at, shards_of):
        steps = jax.random.uniform(jax.random.fold_in(jax.random.fold_in(own_key, 6), axis_at), (shards_of,), jnp.float32, low / len(shards), high / len(shards))
        return jnp.repeat(jnp.exp(steps), shape[axis_at] // shards_of).reshape((-1,) + (1,) * (len(shape) - axis_at - 1))

    factor_of = one(*shards[0])
    for cut in shards[1:]:
        factor_of = factor_of * one(*cut)
    return factor_of


def scatter_about(key, dims, deviation, most, pieces=(), kind=jnp.bfloat16):
    drawn = deviation * jax.random.normal(key, dims, jnp.float32)
    if pieces:
        drawn = drawn * block_scale(key, dims, pieces, -0.22, 0.18)
    return jnp.clip(drawn, -most, most).astype(kind)


def setup_inputs(seed: int = 0) -> dict:
    keys = jax.random.split(jax.random.key(seed), 8)
    return {
        "token_grid": scatter_about(keys[0], (ROWS, D, COLS), 1.0, 6.0, ((0, 8), (1, 4))),
        "norm_gain": jnp.clip(1.0 + 0.18 * jax.random.normal(keys[1], (LAYERS, D), jnp.float32), 0.099609375, 1.8984375).astype(jnp.bfloat16),
        "w_query": scatter_about(keys[2], (LAYERS, D, D), D ** -0.5, 0.125, ((2, 4),)),
        "w_key": scatter_about(keys[3], (LAYERS, D, D), D ** -0.5, 0.125, ((2, 4),)),
        "w_value": scatter_about(keys[4], (LAYERS, D, D), D ** -0.5, 0.125, ((2, 4),)),
        "w_out": scatter_about(keys[5], (LAYERS, D, D), (D // 16) ** -0.5, 0.5, ((1, 4),)),
        "rel_bias": draw_rel_bias(jax.random.fold_in(keys[7], 71), 0),
    }


EPS = 1e-06

def rounded(source):
    return lax.optimization_barrier(source.astype(jnp.bfloat16)).astype(jnp.float32)

def one_layer(token_grid, gain_row, w_query, w_key, w_value, w_out, bias_table):
    grid_wide = token_grid.astype(jnp.float32)
    inverse = lax.rsqrt(lax.optimization_barrier(jnp.mean(grid_wide * grid_wide, axis=1)) + EPS)
    scaled = (grid_wide * gain_row.astype(jnp.float32)[None, :, None]).astype(jnp.bfloat16)
    flat_rows = jnp.transpose(scaled, (0, 2, 1)).reshape(ROWS * COLS, D)
    inverse_flat = inverse.reshape(ROWS * COLS, 1)

    def project(weight):
        product = jnp.dot(flat_rows, weight, preferred_element_type=jnp.float32) * inverse_flat
        return rounded(product).reshape(ROWS, COLS, HEADS, HEAD_DIM)
    queries = project(w_query)
    keys_all = project(w_key)
    values_all = project(w_value)
    factor = HEAD_DIM ** (-0.5)
    offsets = jnp.arange(WIN_R * WIN_C, dtype=jnp.int32)

    def scores_at(offset):
        slot_row = offset // WIN_C
        slot_col = offset % WIN_C
        rolled = jnp.roll(keys_all, (WIN_R // 2 - slot_row, WIN_C // 2 - slot_col), axis=(0, 1))
        offset_bias = lax.dynamic_slice(bias_table, (jnp.int32(0), slot_row, slot_col), (HEADS, 1, 1)).reshape(HEADS)
        return lax.optimization_barrier(jnp.sum(queries * rolled, axis=-1)) * factor + offset_bias
    scores = lax.map(scores_at, offsets)
    weights = rounded(jax.nn.softmax(scores, axis=0))

    def accumulate(running, operands):
        weight_now, offset = operands
        slot_row = offset // WIN_C
        slot_col = offset % WIN_C
        rolled = jnp.roll(values_all, (WIN_R // 2 - slot_row, WIN_C // 2 - slot_col), axis=(0, 1))
        return (running + weight_now[..., None] * rolled, None)
    mixed_out, unused = lax.scan(accumulate, jnp.zeros((ROWS, COLS, HEADS, HEAD_DIM), jnp.float32), (weights, offsets))
    mixed_out = mixed_out.astype(jnp.bfloat16).reshape(ROWS * COLS, N_TP, D // N_TP)
    groups = jnp.moveaxis(mixed_out, 1, 0)
    blocks = w_out.reshape(N_TP, D // N_TP, D)

    def add_group(running, operands):
        partial_value = jnp.dot(operands[0], operands[1], preferred_element_type=jnp.float32)
        return (running + rounded(partial_value), None)
    update, unused = lax.scan(add_group, jnp.zeros((ROWS * COLS, D), jnp.float32), (groups, blocks))
    update = jnp.transpose(update.reshape(ROWS, COLS, D), (0, 2, 1))
    return (grid_wide + update).astype(jnp.bfloat16)

def reference(token_grid, norm_gain, w_query, w_key, w_value, w_out, rel_bias):
    current = token_grid
    for layer_idx in range(LAYERS):
        current = one_layer(current, norm_gain[layer_idx], w_query[layer_idx], w_key[layer_idx], w_value[layer_idx], w_out[layer_idx], rel_bias[layer_idx])
    return current
```

```python
import functools

import jax
import jax.numpy as jnp
from jax import lax
from jax.experimental import pallas as pl
from jax.experimental.pallas import tpu as pltpu
from jax.sharding import PartitionSpec as P

HEAD_DIM = 64
WIN_R = 8
WIN_C = 16
EPS = 1e-06
LANES = 128
NEG = -1e30


def attention_kernel(rows, cols, q_ref, k_ref, v_ref, kh_ref, vh_ref, base_ref, o_ref, tile_ref):
    pack = LANES // cols
    n_slots = min(rows, pack + WIN_R - 1)
    half_r = WIN_R // 2
    span = cols + WIN_C
    lane = lax.broadcasted_iota(jnp.int32, (8, LANES), 1)
    lane_q = lax.broadcasted_iota(jnp.int32, (LANES, LANES), 1)
    v_main = v_ref[...].T
    v_halo = vh_ref[...].T
    neg = jnp.full((8, LANES), NEG, jnp.float32)
    outs = [[] for _ in range(rows * cols // LANES)]
    for head in range(LANES // HEAD_DIM):
        for p in range(pack):
            own = (lane >= p * cols) & (lane < (p + 1) * cols)
            for slot in range(WIN_R):
                e = (slot + p) % rows
                start = jnp.broadcast_to(base_ref[head, slot : slot + 1, :], (8, LANES))
                start = pltpu.roll(start, 0, 1, stride=1, stride_axis=0)
                for blk in range(span // 8):
                    shift = (p * cols + 8 * blk) % LANES
                    moved = pltpu.roll(start, shift, 1) if shift else start
                    at = blk - 1 if 1 <= blk <= cols // 8 else (cols // 8 if blk == 0 else blk)
                    where = pl.ds(e * span + 8 * at, 8)
                    rest = neg if p == 0 and rows == WIN_R else tile_ref[where, :]
                    tile_ref[where, :] = jnp.where(own, moved, rest)
        for group in range(rows * cols // LANES):
            key_rows = [r for r in range(rows) if (r - group * pack + half_r) % rows < n_slots]
            q = q_ref[group * LANES : (group + 1) * LANES, :]
            mine = (lane_q >= head * HEAD_DIM) & (lane_q < (head + 1) * HEAD_DIM)
            q = jnp.where(mine, q, jnp.zeros_like(q))
            s_list = []
            contract = (((1,), (1,)), ((), ()))
            if len(key_rows) == rows:
                s_main = lax.dot_general(k_ref[...], q, contract, preferred_element_type=jnp.float32)
                s_halo = lax.dot_general(kh_ref[...], q, contract, preferred_element_type=jnp.float32)
            main_list = []
            halo_list = []
            for r in key_rows:
                e = (r - group * pack + half_r) % rows
                if len(key_rows) == rows:
                    main = s_main[r * cols : (r + 1) * cols]
                    halo = s_halo[r * WIN_C : (r + 1) * WIN_C]
                else:
                    main = lax.dot_general(
                        k_ref[r * cols : (r + 1) * cols, :], q, contract, preferred_element_type=jnp.float32
                    )
                    halo = lax.dot_general(
                        kh_ref[r * WIN_C : (r + 1) * WIN_C, :], q, contract, preferred_element_type=jnp.float32
                    )
                main_list.append(main + tile_ref[e * span : e * span + cols, :])
                halo_list.append(halo + tile_ref[e * span + cols : (e + 1) * span, :])
            main = jnp.concatenate(main_list, axis=0)
            halo = jnp.concatenate(halo_list, axis=0)
            top = jnp.maximum(jnp.max(main, axis=0, keepdims=True), jnp.max(halo, axis=0, keepdims=True))
            main = jnp.exp(main - top)
            halo = jnp.exp(halo - top)
            total = jnp.sum(main, axis=0, keepdims=True) + jnp.sum(halo, axis=0, keepdims=True)
            main = main.astype(jnp.bfloat16)
            halo = halo.astype(jnp.bfloat16)
            lo = head * HEAD_DIM
            if len(key_rows) == rows:
                vm = v_main[lo : lo + HEAD_DIM]
                vh = v_halo[lo : lo + HEAD_DIM]
            else:
                vm = jnp.concatenate([v_main[lo : lo + HEAD_DIM, r * cols : (r + 1) * cols] for r in key_rows], axis=1)
                vh = jnp.concatenate(
                    [v_halo[lo : lo + HEAD_DIM, r * WIN_C : (r + 1) * WIN_C] for r in key_rows], axis=1
                )
            mixed = jnp.dot(vm, main, preferred_element_type=jnp.float32)
            mixed = mixed + jnp.dot(vh, halo, preferred_element_type=jnp.float32)
            outs[group].append(mixed / total)
    for group in range(rows * cols // LANES):
        both = jnp.concatenate(outs[group], axis=0)
        o_ref[group * LANES : (group + 1) * LANES, :] = both.T.astype(o_ref.dtype)


def attention_kernel_init(rows, cols, *refs):
    tile_ref = refs[-1]
    tile_ref[...] = jnp.full(tile_ref.shape, NEG, jnp.float32)
    attention_kernel(rows, cols, *refs)


def attention(queries, keys, values, halo, base, rows, cols):
    tokens, channels = queries.shape
    n_slots = min(rows, LANES // cols + WIN_R - 1)
    pairs = channels // LANES
    per = LANES // HEAD_DIM
    side = halo.shape[0]
    kernel = attention_kernel if rows == WIN_R else attention_kernel_init
    return pl.pallas_call(
        functools.partial(kernel, rows, cols),
        grid=(pairs,),
        out_shape=jax.ShapeDtypeStruct((tokens, channels), jnp.bfloat16),
        in_specs=[
            pl.BlockSpec((tokens, LANES), lambda i: (0, i)),
            pl.BlockSpec((tokens, LANES), lambda i: (0, i)),
            pl.BlockSpec((tokens, LANES), lambda i: (0, i)),
            pl.BlockSpec((side, LANES), lambda i: (0, i)),
            pl.BlockSpec((side, LANES), lambda i: (0, i + pairs)),
            pl.BlockSpec((per, WIN_R, LANES), lambda i: (i, 0, 0)),
        ],
        out_specs=pl.BlockSpec((tokens, LANES), lambda i: (0, i)),
        scratch_shapes=[pltpu.VMEM((n_slots * (cols + WIN_C), LANES), jnp.float32)],
        compiler_params=pltpu.CompilerParams(vmem_limit_bytes=48 * 1024 * 1024),
        name="window_attention",
    )(queries, keys, values, halo, halo, base)


def body(token_grid, norm_gain, w_query, w_key, w_value, w_out, rel_bias):
    n = lax.axis_size("sp")
    rows_dev, channels, columns = token_grid.shape
    rows = rows_dev * n
    cols = columns // n
    tokens = rows * cols
    width = norm_gain.shape[1]
    factor = HEAD_DIM ** (-0.5)
    half_c = WIN_C // 2
    base = jnp.concatenate(
        [
            rel_bias[..., :1],
            jnp.full(rel_bias.shape[:-1] + (LANES - WIN_C,), NEG, jnp.float32),
            jnp.flip(rel_bias[..., 1:], axis=-1),
        ],
        axis=-1,
    )
    turned = jnp.transpose(token_grid, (2, 0, 1)).reshape(columns, rows_dev * channels)
    current = lax.all_to_all(turned, "sp", split_axis=0, concat_axis=0, tiled=True)
    to_right = [(i, (i + 1) % n) for i in range(n)]
    to_left = [(i, (i - 1) % n) for i in range(n)]
    for layer in range(norm_gain.shape[0]):
        gain = norm_gain[layer].astype(jnp.float32)
        raw = lax.all_gather(current, "tp", axis=1, tiled=True).astype(jnp.float32)
        scaled = (raw * gain[None, :]).astype(jnp.bfloat16)
        inverse = lax.rsqrt(jnp.sum(raw * raw, axis=1, keepdims=True) / width + EPS)

        def project(weight, scale=1.0):
            product = jnp.dot(scaled, weight[layer], preferred_element_type=jnp.float32)
            return (product * inverse).astype(jnp.bfloat16) * jnp.bfloat16(scale)

        keys = project(w_key)
        values = project(w_value)
        keyval = jnp.concatenate([keys, values], axis=1).reshape(rows, cols, 2 * channels)
        left = lax.ppermute(keyval[:, cols - half_c :], "sp", to_right)
        right = lax.ppermute(keyval[:, :half_c], "sp", to_left)
        queries = project(w_query, factor)
        halo = jnp.concatenate([left, right], axis=1).reshape(rows * WIN_C, 2 * channels)
        mixed = attention(queries, keys, values, halo, base[layer], rows, cols)
        partial = jnp.dot(mixed, w_out[layer], preferred_element_type=jnp.float32).astype(jnp.bfloat16)
        update = lax.psum_scatter(partial, "tp", scatter_dimension=1, tiled=True)
        current = (current.astype(jnp.float32) + update.astype(jnp.float32)).astype(jnp.bfloat16)
    back = lax.all_to_all(current, "sp", split_axis=0, concat_axis=0, tiled=True)
    return jnp.transpose(back.reshape(columns, rows_dev, channels), (1, 2, 0))


def solution(mesh):
    in_specs = (
        P("sp", "tp", None),
        P(),
        P(None, None, "tp"),
        P(None, None, "tp"),
        P(None, None, "tp"),
        P(None, "tp", None),
        P(None, "tp", None, None),
    )
    out_specs = P("sp", "tp", None)
    return jax.shard_map(body, mesh=mesh, in_specs=in_specs, out_specs=out_specs, check_vma=False)
```
